128 devices in a mesh: rep: 2 (over z_hi), fs: 32 (over z_lo, y, x), tp: 2 (over core).
Axes of the slice: x: 4, y: 4, z: 4 (z_hi: 2, z_lo: 2; z = z_hi * 2 + z_lo), core: 2. Of those that a mesh axis runs over, the one named last changes fastest.
Arguments:
- tokens: bfloat16 [40960, 2048], P(('rep', 'fs'), 'tp'), may hold values from -6 to 6
- norm_first: float32 [2048], replicated, may hold values from 0.1 to 1.9
- norm_mix: float32 [2048], replicated, may hold values from 0.1 to 1.9
- norm_second: float32 [2048], replicated, may hold values from 0.1 to 1.9
- gate_weight: float32 [2048, 2816], P('fs', 'tp'), may hold values from -0.125 to 0.125
- up_weight: float32 [2048, 2816], P('fs', 'tp'), may hold values from -0.125 to 0.125
- down_weight: float32 [2816, 2048], P('tp', 'fs'), may hold values from -0.109375 to 0.109375
- gate_scale: float32 [2816], P('tp'), may hold values from 0.3 to 3
- up_scale: float32 [2816], P('tp'), may hold values from 0.3 to 3
- down_scale: float32 [2048], P('fs'), may hold values from 0.3 to 3
- u_weight: float32 [2048, 1024], P('fs', 'tp'), may hold values from -0.125 to 0.125
- v_weight: float32 [2048, 1024], P('fs', 'tp'), may hold values from -0.125 to 0.125
- u_scale: float32 [1024], P('tp'), may hold values from 0.3 to 3
- v_scale: float32 [1024], P('tp'), may hold values from 0.15 to 6
- ln_gain: float32 [1024], P('tp'), may hold values from 0.1 to 1.9
- ln_bias: float32 [1024], P('tp'), may hold values from -3 to 3
- spatial_weight: bfloat16 [8, 128, 128], P('tp'), may hold values from -0.25 to 0.25
- spatial_bias: float32 [8, 128], P('tp'), may hold values from 0.1 to 1.9
- out_weight: float32 [1024, 2048], P('tp', 'fs'), may hold values from -0.1875 to 0.1875
- out_scale: float32 [2048], P('fs'), may hold values from 0.3 to 3
Outputs:
- layer_out: bfloat16 [40960, 2048], P(('rep', 'fs'), 'tp')
The draws below stay inside these ranges and needn't reach their ends.
All inputs are finite; a program needn't handle non-finite values.
Results may differ from the reference program's by a relative error of at most 0.019.
Values may be sent and summed in bfloat16 or wider, within the bound.
A program may use at most 128 MiB of HBM per device.

```python
import math
import jax
import jax.numpy as jnp
from jax import lax

D = 2048
FF = 2816
BW = 1024
SPAN = 128
GROUPS = 8
TOKENS = 40960
N_TP = 2


def draw_v_scale(key, part):
    position = jnp.arange(BW, dtype=jnp.float32) / (BW - 1)
    rough = jax.random.uniform(key, (BW,), jnp.float32, 0.6, 1.4)
    return (10.0 ** (position - 0.5) * rough).astype(jnp.float32)


def steps_of(key, shape, pieces, least, largest):
    level = 1.0
    for dim, blocks in pieces:
        draws = jax.random.uniform(jax.random.fold_in(jax.random.fold_in(key, 6), dim), (blocks,), jnp.float32, least / len(pieces), largest / len(pieces))
        level = level * jnp.repeat(jnp.exp(draws), shape[dim] // blocks).reshape((-1,) + (1,) * (len(shape) - 1 - dim))
    return level


def centred(rng, dims, deviation, limit, split=(), kind=jnp.bfloat16):
    values = deviation * jax.random.normal(rng, dims, jnp.float32)
    if split:
        values = values * steps_of(rng, dims, split, -0.22, 0.18)
    return jnp.clip(values, -limit, limit).astype(kind)


def setup_inputs(seed: int = 0) -> dict:
    splits = jax.random.split(jax.random.key(seed), 21)
    return {
        "tokens": centred(splits[0], (TOKENS, D), 1.0, 6.0, ((0, 64), (1, 2))),
        "norm_first": jnp.clip(1.0 + 0.18 * jax.random.normal(splits[1], (D,), jnp.float32), 0.1, 1.9),
        "norm_mix": jnp.clip(1.0 + 0.18 * jax.random.normal(splits[2], (D,), jnp.float32), 0.1, 1.9),
        "norm_second": jnp.clip(1.0 + 0.18 * jax.random.normal(splits[3], (D,), jnp.float32), 0.1, 1.9),
        "gate_weight": centred(splits[4], (D, FF), D ** -0.5, 0.125, ((0, 32), (1, 2)), jnp.float32),
        "up_weight": centred(splits[5], (D, FF), D ** -0.5, 0.125, ((0, 32), (1, 2)), jnp.float32),
        "down_weight": centred(splits[6], (FF, D), FF ** -0.5, 0.109375, ((0, 2), (1, 32)), jnp.float32),
        "gate_scale": jnp.clip(jnp.exp(math.log(3.0) - 2.3025851 * jax.random.uniform(splits[7], (FF,), jnp.float32) ** steps_of(splits[7], (FF,), ((0, 2),), -0.2, 0.2)), 0.3, 3.0),
        "up_scale": jnp.clip(jnp.exp(math.log(3.0) - 2.3025851 * jax.random.uniform(splits[8], (FF,), jnp.float32) ** steps_of(splits[8], (FF,), ((0, 2),), -0.2, 0.2)), 0.3, 3.0),
        "down_scale": jnp.clip(jnp.exp(math.log(3.0) - 2.3025851 * jax.random.uniform(splits[9], (D,), jnp.float32) ** steps_of(splits[9], (D,), ((0, 32),), -0.2, 0.2)), 0.3, 3.0),
        "u_weight": centred(splits[10], (D, BW), D ** -0.5, 0.125, ((0, 32), (1, 2)), jnp.float32),
        "v_weight": centred(splits[11], (D, BW), D ** -0.5, 0.125, ((0, 32), (1, 2)), jnp.float32),
        "u_scale": jnp.clip(jnp.exp(math.log(3.0) - 2.3025851 * jax.random.uniform(splits[12], (BW,), jnp.float32) ** steps_of(splits[12], (BW,), ((0, 2),), -0.2, 0.2)), 0.3, 3.0),
        "v_scale": draw_v_scale(jax.random.fold_in(splits[20], 71), 0),
        "ln_gain": jnp.clip(1.0 + 0.18 * jax.random.normal(splits[14], (BW,), jnp.float32), 0.1, 1.9),
        "ln_bias": centred(splits[15], (BW,), 0.5, 3.0, ((0, 2),), jnp.float32),
        "spatial_weight": centred(splits[16], (GROUPS, SPAN, SPAN), (4 * SPAN) ** -0.5, 0.25, ((0, 2),)),
        "spatial_bias": jnp.clip(1.0 + 0.18 * jax.random.normal(splits[17], (GROUPS, SPAN), jnp.float32), 0.1, 1.9),
        "out_weight": centred(splits[18], (BW, D), BW ** -0.5, 0.1875, ((0, 2), (1, 32)), jnp.float32),
        "out_scale": jnp.clip(jnp.exp(math.log(3.0) - 2.3025851 * jax.random.uniform(splits[19], (D,), jnp.float32) ** steps_of(splits[19], (D,), ((0, 32),), -0.2, 0.2)), 0.3, 3.0),
    }


EPS = 1e-06

def rms_norm(rows, gain):
    values = rows.astype(jnp.float32)
    scale = lax.rsqrt(lax.optimization_barrier(jnp.mean(values * values, axis=1, keepdims=True)) + EPS)
    return (values * scale * gain).astype(jnp.bfloat16)

def project(left, weight, scale):
    return jnp.dot(left, weight.astype(jnp.bfloat16), preferred_element_type=jnp.float32) * scale

def block_sum(left, weight, scale):
    width = left.shape[1] // N_TP
    total = jnp.zeros((left.shape[0], weight.shape[1]), jnp.float32)
    for index in range(N_TP):
        partial_term = project(left[:, index * width:(index + 1) * width], weight[index * width:(index + 1) * width], scale)
        partial_term = lax.optimization_barrier(partial_term.astype(jnp.bfloat16))
        total = total + partial_term.astype(jnp.float32)
    return total

def feed_forward(normed, gate_weight, up_weight, down_weight, gate_scale, up_scale, down_scale):
    gate = project(normed, gate_weight, gate_scale)
    up_part = project(normed, up_weight, up_scale)
    hidden = (jax.nn.silu(gate) * up_part).astype(jnp.bfloat16)
    return block_sum(hidden, down_weight, down_scale)

def reference(tokens, norm_first, norm_mix, norm_second, gate_weight, up_weight, down_weight, gate_scale, up_scale, down_scale, u_weight, v_weight, u_scale, v_scale, ln_gain, ln_bias, spatial_weight, spatial_bias, out_weight, out_scale):
    first = feed_forward(rms_norm(tokens, norm_first), gate_weight, up_weight, down_weight, gate_scale, up_scale, down_scale)
    middle = (tokens.astype(jnp.float32) + 0.5 * first).astype(jnp.bfloat16)
    mix_normed = rms_norm(middle, norm_mix)
    u_pre = project(mix_normed, u_weight, u_scale)
    v_pre = project(mix_normed, v_weight, v_scale)
    v_act = jax.nn.gelu(v_pre, approximate=True)
    v_mean = lax.optimization_barrier(jnp.mean(v_act, axis=1, keepdims=True))
    v_var = lax.optimization_barrier(jnp.mean(v_act * v_act, axis=1, keepdims=True)) - v_mean * v_mean
    v_normed = ((v_act - v_mean) * lax.rsqrt(v_var + EPS) * ln_gain + ln_bias).astype(jnp.bfloat16)
    count = tokens.shape[0]
    groups = spatial_weight.shape[0]
    blocks = v_normed.reshape(count // SPAN, SPAN, groups, BW // groups).astype(jnp.float32)
    lower = jnp.tril(jnp.ones((SPAN, SPAN), jnp.float32))
    masked = (spatial_weight.astype(jnp.float32) * lower[None]).astype(jnp.float32)
    spatial = jnp.einsum('gts,nsgc->ntgc', masked, blocks) + spatial_bias.T[None, :, :, None]
    mixed = (jax.nn.gelu(u_pre, approximate=True) * spatial.reshape(count, BW)).astype(jnp.bfloat16)
    second = (middle.astype(jnp.float32) + block_sum(mixed, out_weight, out_scale)).astype(jnp.bfloat16)
    last = feed_forward(rms_norm(second, norm_second), gate_weight, up_weight, down_weight, gate_scale, up_scale, down_scale)
    return (second.astype(jnp.float32) + 0.5 * last).astype(jnp.bfloat16)
```

```python
import functools

import jax
import jax.numpy as jnp
from jax import lax
from jax.experimental import pallas as pl
from jax.experimental.pallas import tpu as pltpu
from jax.sharding import Mesh
from jax.sharding import PartitionSpec as P

BW = 1024
SPAN = 128
EPS = 1e-06
FS = ("fs_0", "fs_1", "fs_2")
REP_FS = ("rep", "fs_0", "fs_1", "fs_2")
MESH = pl.DeviceIdType.MESH
BF = jnp.bfloat16
F32 = jnp.float32

N_UNITS = 23
NARROW = 16
ROUTES = (
    1, 0, 0, 1, 0, 3, 2, 2, 1, 2, 0, 1, 1, 3, 3, 3, 1, 0, 2, 0, 3, 0, 3,
)
PROGRAM = (
    0, 10, 20, 30, 40, 50, 60, 1090, 1, 11, 21, 31, 41, 51, 61, 70, 80, 90, 100, 110, 2, 12, 120,
    32, 22, 130, 71, 42, 140, 150, 91, 160, 52, 170, 62, 81, 101, 131, 111, 141, 151, 3, 13, 121,
    33, 23, 72, 92, 171, 43, 161, 63, 102, 53, 82, 4, 132, 112, 34, 73, 142, 93, 172, 152, 14,
    122, 24, 5, 180, 1100, 44, 54, 162, 83, 35, 190, 1103, 64, 113, 103, 123, 133, 15, 200, 1101,
    55, 210, 1105, 163, 84, 74, 191, 143, 25, 220, 1102, 114, 181, 124, 94, 45, 1104, 201, 134,
    173, 211, 153, 164, 192, 65, 1106, 85, 1108, 104, 221, 144, 75, 1107, 182, 115, 95, 1109,
    135, 212, 202, 174, 125, 193, 154, 222, 165, 145, 213, 183, 203, 194, 223, 155, 105, 1110,
    214, 1120, 1121, 1122, 1123, 1124, 1125, 204, 1126, 1127, 175, 184, 1130, 1131, 224, 185,
    1140, 195, 1141, 205, 1150, 1151, 1160, 225, 1161, 215, 1170, 1171,
)

GROUPS_OF_ROWS = ((0, 384), (384, 256))
STEP_ROWS = 32


def gelu(a):
    return 0.5 * a * (1.0 + jnp.tanh(0.7978845608028654 * (a + 0.044715 * (a * a * a))))


def silu(a):
    return 0.5 * a * (1.0 + jnp.tanh(0.5 * a))


def dot(a, b):
    return jnp.dot(a, b, preferred_element_type=F32)


def dot_t(a, b):
    return lax.dot_general(a, b, (((1,), (1,)), ((), ())), preferred_element_type=F32)


def kernel(
    tokens, norm_first, norm_mix, norm_second, gate_w, up_w, down_w, gate_s, up_s, down_s,
    u_w, v_w, u_s, v_s, ln_gain, ln_bias, spatial_w, spatial_b, out_w, out_s,
    result,
    wide, narrow, whole, normed, middle, hidden, part, got_first, got_mix, last_part, got_last,
    u_act, v_act, mixed, stats, stats_got,
    sent, arrived, pair_sent, pair_arrived,
):
    rep, z, y, x, tp = (lax.axis_index(a) for a in ("rep", "fs_0", "fs_1", "fs_2", "tp"))
    xp, xm = lax.rem(x + 1, 4), lax.rem(x + 3, 4)
    yp, ym = lax.rem(y + 1, 4), lax.rem(y + 3, 4)
    full_z = rep * 2 + z
    zp, zm = lax.rem(full_z + 1, 4), lax.rem(full_z + 3, 4)
    to_xp, to_xm = {"fs_2": xp}, {"fs_2": xm}
    to_yp, to_ym = {"fs_1": yp}, {"fs_1": ym}
    to_zp = {"rep": zp // 2, "fs_0": lax.rem(zp, 2)}
    to_zm = {"rep": zm // 2, "fs_0": lax.rem(zm, 2)}
    partner = {"tp": 1 - tp}

    def unit(u):
        return narrow if u == NARROW else wide.at[u if u < NARROW else u - 1]

    def place(u, value):
        if u == NARROW:
            narrow[z, y, x] = value.astype(BF)
        else:
            wide[u if u < NARROW else u - 1, z, y, x] = value.astype(BF)

    for i in range(11):
        cols, row = slice(128 * i, 128 * i + 128), slice(i, i + 1)
        place(i, jnp.concatenate([gate_w[:, cols] * gate_s[row], up_w[:, cols] * up_s[row]], axis=1))
    diagonal = lax.broadcasted_iota(jnp.int32, (64, 64), 0) == lax.broadcasted_iota(
        jnp.int32, (64, 64), 1)

    def upright(ref):
        return jnp.sum(jnp.where(diagonal, ref[...], 0.0), axis=1, keepdims=True)

    down_scale, out_scale = upright(down_s), upright(out_s)
    for j in range(5):
        place(11 + j, down_w[:, 256 * j : 256 * j + 256] * down_scale)
    place(NARROW, down_w[:, 1280:1408] * down_scale)
    for j in range(2):
        cols = slice(256 * j, 256 * j + 256)
        place(17 + j, v_w[:, cols] * v_s[:, cols])
        place(19 + j, u_w[:, cols] * u_s[:, cols])
        place(21 + j, out_w[:, cols] * out_scale)
    whole[tp] = tokens[...]

    barrier = pltpu.get_barrier_semaphore()
    for other in (to_xp, to_xm, to_yp, to_ym, to_zp, to_zm, partner):
        pl.semaphore_signal(barrier, inc=1, device_id=other, device_id_type=MESH)
    pl.semaphore_wait(barrier, 7)

    def send(ref, to, u, k):
        pltpu.make_async_remote_copy(
            src_ref=ref, dst_ref=ref, send_sem=sent.at[u, k], recv_sem=arrived.at[u, k],
            device_id=to, device_id_type=MESH,
        ).start()

    def region(u, k):
        b = unit(u)
        if ROUTES[u] < 2:
            return (b.at[0, 0, 0:2], b.at[0, 0, 0], b.at[0, 0:2], b.at[0, 0], b.at[0])[k]
        return (b.at[0, 0, 0], b.at[0, 0], b.at[0, 0, 0:2], b.at[0], b.at[0, 0:2])[k]

    def wait_for(u, k, sems):
        ref = region(u, k)
        pltpu.make_async_copy(ref, ref, sems.at[u, k]).wait()

    def step(u, k):
        if k > 0:
            wait_for(u, k - 1, arrived)
        b, route = unit(u), ROUTES[u]
        if k == 5:
            return
        if route == 0:
            refs = (
                ((b.at[z, y, x], to_xp), (b.at[z, y, x], to_xm)),
                ((b.at[z, y, xm, 0:32], to_xp), (b.at[z, y, xp, 32:64], to_xm)),
                ((b.at[z, y], to_yp), (b.at[z, y], to_ym)),
                ((b.at[z, ym, 0:2], to_yp), (b.at[z, yp, 2:4], to_ym)),
                ((b.at[z, 0:2], to_zp), (b.at[z, 2:4], to_zm)),
            )
        elif route == 1:
            refs = (
                ((b.at[z, y, x], to_yp), (b.at[z, y, x], to_ym)),
                ((b.at[z, ym, x, 0:32], to_yp), (b.at[z, yp, x, 32:64], to_ym)),
                ((b.at[z, :, x], to_xp), (b.at[z, :, x], to_xm)),
                ((b.at[z, 0:2, xm], to_xp), (b.at[z, 2:4, xp], to_xm)),
                ((b.at[z, 0:2], to_zp), (b.at[z, 2:4], to_zm)),
            )
        elif route == 2:
            refs = (
                ((b.at[z, y, x, 0:32], to_zp), (b.at[z, y, x, 32:64], to_zm)),
                ((b.at[:, y, x], to_xp), (b.at[:, y, x], to_xm)),
                ((b.at[0, y, xm], to_xp), (b.at[1, y, xp], to_xm)),
                ((b.at[:, y], to_yp), (b.at[:, y], to_ym)),
                ((b.at[0, ym], to_yp), (b.at[1, yp], to_ym)),
            )
        else:
            refs = (
                ((b.at[z, y, x, 0:32], to_zp), (b.at[z, y, x, 32:64], to_zm)),
                ((b.at[:, y, x], to_yp), (b.at[:, y, x], to_ym)),
                ((b.at[0, ym, x], to_yp), (b.at[1, yp, x], to_ym)),
                ((b.at[:, :, x], to_xp), (b.at[:, :, x], to_xm)),
                ((b.at[0, :, xm], to_xp), (b.at[1, :, xp], to_xm)),
            )
        for ref, to in refs[k]:
            send(ref, to, u, k)

    def pair(src, dst, n):
        return pltpu.make_async_remote_copy(
            src_ref=src, dst_ref=dst, send_sem=pair_sent.at[n], recv_sem=pair_arrived.at[n],
            device_id=partner, device_id_type=MESH,
        )

    def rows_of(h):
        at, size = GROUPS_OF_ROWS[h]
        return pl.ds(at, size)

    exchange_tokens = pair(tokens, whole.at[tp], 0)
    exchange_tokens.start()
    exchange_first = [pair(part.at[rows_of(h)], got_first.at[rows_of(h)], 1 + h) for h in (0, 1)]
    exchange_stats = [pair(stats.at[rows_of(h)], stats_got.at[rows_of(h)], 3 + h) for h in (0, 1)]
    exchange_mix = [pair(part.at[rows_of(h)], got_mix.at[rows_of(h)], 5 + h) for h in (0, 1)]
    exchange_last = [
        pair(last_part.at[rows_of(h)], got_last.at[rows_of(h)], 7 + h) for h in (0, 1)
    ]

    def by_rows(at, size, step_rows, body):
        def one(i, carry):
            body(pl.ds(pl.multiple_of(at + i * step_rows, step_rows), step_rows))
            return carry

        lax.fori_loop(0, size // step_rows, one, 0)

    def normalise(values, gain):
        factor = lax.rsqrt(jnp.mean(values * values, axis=1, keepdims=True) + EPS)
        return (values * factor * gain[...]).astype(BF)

    def norm_tokens():
        exchange_tokens.wait()

        def body(r):
            values = jnp.concatenate([whole[0, r], whole[1, r]], axis=1).astype(F32)
            normed[r] = normalise(values, norm_first)

        by_rows(0, 640, STEP_ROWS, body)

    def gate_up(u, at, size):
        r = pl.ds(at, size)
        both = dot(normed[r], wide[u].reshape(2048, 256))
        hidden[u, r] = (silu(both[:, :128]) * both[:, 128:]).astype(BF)

    def first_hidden(u):
        def one(i, carry):
            gate_up(u, pl.multiple_of(i * 320, 320), 320)
            return carry

        lax.fori_loop(0, 2, one, 0)

    def down_rows(h, zi, yi):
        r = rows_of(h)
        left = jnp.concatenate([hidden[i, r] for i in range(11)], axis=1)
        right = jnp.concatenate(
            [wide[11 + j, zi, pl.ds(yi, 2)].reshape(512, 256) for j in range(5)]
            + [narrow[zi, pl.ds(yi, 2)].reshape(512, 128)], axis=1)
        return dot_t(left, right)

    def first_down(h, nb):
        part[rows_of(h), 512 * nb : 512 * nb + 512] = down_rows(h, nb // 2, 2 * (nb % 2)).astype(BF)
        if nb == 3:
            exchange_first[h].start()

    def combine_first(h):
        exchange_first[h].wait()

        def body(r):
            values = jnp.concatenate([whole[0, r], whole[1, r]], axis=1).astype(F32)
            branch = part[r].astype(F32) + got_first[r].astype(F32)
            total = (values + 0.5 * branch).astype(BF)
            middle[r] = total
            normed[r] = normalise(total.astype(F32), norm_mix)

        by_rows(*GROUPS_OF_ROWS[h], STEP_ROWS, body)

    def project_v(h):
        r = rows_of(h)
        lane = lax.broadcasted_iota(jnp.int32, (GROUPS_OF_ROWS[h][1], 128), 1)
        total = total_sq = 0.0
        for j in range(2):
            act = gelu(dot(normed[r], wide[16 + j].reshape(2048, 256)))
            v_act[r, 256 * j : 256 * j + 256] = act
            total += jnp.sum(act, axis=1, keepdims=True)
            total_sq += jnp.sum(act * act, axis=1, keepdims=True)
        stats[r] = jnp.where(lane == 0, total, jnp.where(lane == 1, total_sq, 0.0))
        exchange_stats[h].start()

    def project_u(h):
        r = rows_of(h)
        for j in range(2):
            act = gelu(dot(normed[r], wide[18 + j].reshape(2048, 256)))
            u_act[r, 256 * j : 256 * j + 256] = act

    def mix(h):
        exchange_stats[h].wait()
        row = lax.broadcasted_iota(jnp.int32, (SPAN, SPAN), 0)
        col = lax.broadcasted_iota(jnp.int32, (SPAN, SPAN), 1)

        def body(r):
            sums = stats[r] + stats_got[r]
            mean = sums[:, 0:1] * (1.0 / BW)
            var = sums[:, 1:2] * (1.0 / BW) - mean * mean
            factor = lax.rsqrt(var + EPS)
            for g in range(4):
                c = slice(128 * g, 128 * g + 128)
                v = ((v_act[r, c] - mean) * factor * ln_gain[:, c] + ln_bias[:, c]).astype(BF)
                w = jnp.where(col <= row, spatial_w[g].astype(F32), 0.0).astype(BF)
                bias = jnp.sum(
                    jnp.where(col == row, spatial_b[g : g + 1, :], 0.0), axis=1, keepdims=True)
                spatial = dot(w, v) + bias
                mixed[r, c] = (u_act[r, c] * spatial).astype(BF)

        by_rows(*GROUPS_OF_ROWS[h], SPAN, body)

    def project_out(h):
        r = rows_of(h)

        def one(nb, carry):
            zi, yi = nb // 2, 2 * lax.rem(nb, 2)
            right = jnp.concatenate(
                [wide[20 + j, zi, pl.ds(yi, 2)].reshape(512, 256) for j in range(2)], axis=1)
            cols = pl.ds(pl.multiple_of(512 * nb, 512), 512)
            part[r, cols] = dot_t(mixed[r], right).astype(BF)
            return carry

        lax.fori_loop(0, 4, one, 0)
        exchange_mix[h].start()

    def combine_mix(h):
        exchange_mix[h].wait()

        def body(r):
            branch = part[r].astype(F32) + got_mix[r].astype(F32)
            total = (middle[r].astype(F32) + branch).astype(BF)
            middle[r] = total
            normed[r] = normalise(total.astype(F32), norm_second)

        by_rows(*GROUPS_OF_ROWS[h], STEP_ROWS, body)

    def second_hidden(h):
        at, size = GROUPS_OF_ROWS[h]

        def one(u, carry):
            gate_up(u, at, size)
            return carry

        lax.fori_loop(0, 11, one, 0)

    def second_down(h):
        r = rows_of(h)
        for nb in range(2):
            c = slice(512 * nb, 512 * nb + 512)
            last_part[r, c] = down_rows(h, 1 - tp, 2 * nb).astype(BF)
        exchange_last[h].start()
        for nb in range(2):
            c = slice(512 * nb, 512 * nb + 512)
            part[r, c] = down_rows(h, tp, 2 * nb).astype(BF)

    def finish(h):
        exchange_last[h].wait()

        def body(r):
            own = middle[r, pl.ds(pl.multiple_of(tp * 1024, 1024), 1024)].astype(F32)
            branch = part[r, 0:1024].astype(F32) + got_last[r].astype(F32)
            result[r] = (own + 0.5 * branch).astype(BF)

        by_rows(*GROUPS_OF_ROWS[h], STEP_ROWS, body)

    def task(n):
        if n == 90:
            norm_tokens()
        elif n < 120:
            first_hidden(n - 100)
        elif n < 130:
            first_down((n - 120) // 4, n % 4)
        else:
            run = (combine_first, project_v, project_u, mix, project_out)
            run[n // 10 - 13](n % 10)

    for code in PROGRAM:
        if code < 1000:
            step(code // 10, code % 10)
        else:
            task(code - 1000)
    for h in (0, 1):
        combine_mix(h)
        second_hidden(h)
        second_down(h)
    for h in (0, 1):
        finish(h)
    for u in range(N_UNITS):
        for k in range(5):
            wait_for(u, k, sent)


def on_device(*args):
    (tokens, norm_first, norm_mix, norm_second, gate_w, up_w, down_w, gate_s, up_s, down_s,
     u_w, v_w, u_s, v_s, ln_gain, ln_bias, spatial_w, spatial_b, out_w, out_s) = args
    line = lambda a: a.reshape(1, -1)
    rows = tokens.shape[0]
    vmem = pltpu.VMEM
    return pl.pallas_call(
        kernel,
        out_shape=jax.ShapeDtypeStruct(tokens.shape, BF),
        in_specs=[pl.BlockSpec(memory_space=pltpu.VMEM)] * 20,
        out_specs=pl.BlockSpec(memory_space=pltpu.VMEM),
        scratch_shapes=[
            vmem((N_UNITS - 1, 2, 4, 4, 64, 256), BF),
            vmem((2, 4, 4, 64, 128), BF),
            vmem((2, rows, 1024), BF),
            vmem((rows, 2048), BF),
            vmem((rows, 2048), BF),
            vmem((11, rows, 128), BF),
            vmem((rows, 2048), BF),
            vmem((rows, 2048), BF),
            vmem((rows, 2048), BF),
            vmem((rows, 1024), BF),
            vmem((rows, 1024), BF),
            vmem((rows, 512), F32),
            vmem((rows, 512), F32),
            vmem((rows, 512), BF),
            vmem((rows, 128), F32),
            vmem((rows, 128), F32),
            pltpu.SemaphoreType.DMA((N_UNITS, 5)),
            pltpu.SemaphoreType.DMA((N_UNITS, 5)),
            pltpu.SemaphoreType.DMA((9,)),
            pltpu.SemaphoreType.DMA((9,)),
        ],
        compiler_params=pltpu.CompilerParams(
            collective_id=0, has_side_effects=True, vmem_limit_bytes=67043328
        ),
    )(tokens, line(norm_first), line(norm_mix), line(norm_second), gate_w, up_w, down_w.T,
      gate_s.reshape(-1, 128), up_s.reshape(-1, 128), line(down_s), u_w, v_w, line(u_s), line(v_s), line(ln_gain),
      line(ln_bias), spatial_w, spatial_b, out_w.T, line(out_s))


def solution(mesh):
    torus = Mesh(
        mesh.devices.reshape(mesh.shape["rep"], 2, 4, 4, mesh.shape["tp"]),
        ("rep", "fs_0", "fs_1", "fs_2", "tp"),
    )
    in_specs = (
        P(REP_FS, "tp"), P(), P(), P(), P(FS, "tp"), P(FS, "tp"), P("tp", FS), P("tp"), P("tp"),
        P(FS), P(FS, "tp"), P(FS, "tp"), P("tp"), P("tp"), P("tp"), P("tp"),
        P("tp", None, None), P("tp", None), P("tp", FS), P(FS),
    )
    return jax.shard_map(
        on_device, mesh=torus, in_specs=in_specs, out_specs=P(REP_FS, "tp"), check_vma=False
    )
```

```python
import functools

import jax
import jax.numpy as jnp
from jax import lax
from jax.experimental import pallas as pl
from jax.experimental.pallas import tpu as pltpu
from jax.sharding import Mesh
from jax.sharding import PartitionSpec as P

BW = 1024
SPAN = 128
EPS = 1e-06
FS = ("fs_0", "fs_1", "fs_2")
REP_FS = ("rep", "fs_0", "fs_1", "fs_2")
MESH = pl.DeviceIdType.MESH
BF = jnp.bfloat16
F32 = jnp.float32

N_UNITS = 23
NARROW = 16
ROUTES = (
    0, 0, 4, 1, 5, 5, 1, 2, 1, 0, 1, 4, 1, 4, 4, 5, 0, 1, 1, 2, 3, 5, 2,
)
PROGRAM = (
    60, 90, 100, 150, 0, 40, 160, 130, 61, 80, 91, 50, 101, 20, 10, 151, 1, 140, 161, 120, 41,
    1090, 62, 92, 131, 81, 51, 21, 102, 30, 11, 152, 70, 2, 170, 121, 110, 141, 162, 42, 153, 71,
    63, 93, 132, 82, 22, 52, 43, 31, 103, 133, 12, 3, 111, 142, 171, 23, 122, 53, 163, 94, 143,
    32, 154, 72, 64, 134, 95, 180, 1109, 83, 13, 4, 172, 65, 190, 1106, 44, 104, 112, 24, 164,
    123, 5, 220, 1100, 191, 144, 54, 105, 210, 1110, 135, 200, 181, 113, 33, 14, 165, 155, 221,
    201, 73, 25, 1102, 84, 145, 211, 182, 173, 15, 1101, 45, 1104, 124, 114, 192, 85, 1108, 202,
    55, 1105, 34, 222, 125, 74, 212, 183, 174, 115, 193, 203, 223, 35, 1103, 184, 75, 1107, 213,
    1120, 1121, 1122, 1123, 1124, 1125, 1126, 204, 1127, 194, 175, 1130, 1131, 214, 224, 185,
    1140, 1141, 205, 195, 1150, 1151, 1160, 215, 1161, 225, 1170, 1171,
)

GROUPS_OF_ROWS = ((0, 384), (384, 256))
STEP_ROWS = 16
UNROLL = 8
PLACED_AHEAD = 4


def gelu(a):
    return 0.5 * a * (1.0 + jnp.tanh(0.7978845608028654 * (a + 0.044715 * (a * a * a))))


def silu(a):
    return 0.5 * a * (1.0 + jnp.tanh(0.5 * a))


def dot(a, b):
    return jnp.dot(a, b, preferred_element_type=F32)


def dot_t(a, b):
    return lax.dot_general(a, b, (((1,), (1,)), ((), ())), preferred_element_type=F32)


def kernel(
    tokens, norm_first, norm_mix, norm_second, gate_hbm, up_hbm, down_hbm, gate_s, up_s, down_s,
    u_hbm, v_hbm, u_s, v_s, ln_gain, ln_bias, spatial_w, spatial_b, out_hbm, out_s,
    result,
    gate_w, up_w, down_w, v_w, u_w, out_w,
    wide, narrow, whole, normed, middle, hidden, part, got_first, got_mix, last_part, got_last,
    u_act, v_act, mixed, stats, stats_got,
    sent, arrived, pair_sent, pair_arrived, load_sem, store_sem,
):
    rep, z, y, x, tp = (lax.axis_index(a) for a in ("rep", "fs_0", "fs_1", "fs_2", "tp"))
    xp, xm = lax.rem(x + 1, 4), lax.rem(x + 3, 4)
    yp, ym = lax.rem(y + 1, 4), lax.rem(y + 3, 4)
    full_z = rep * 2 + z
    zp, zm = lax.rem(full_z + 1, 4), lax.rem(full_z + 3, 4)
    to_xp, to_xm = {"fs_2": xp}, {"fs_2": xm}
    to_yp, to_ym = {"fs_1": yp}, {"fs_1": ym}
    to_zp = {"rep": zp // 2, "fs_0": lax.rem(zp, 2)}
    to_zm = {"rep": zm // 2, "fs_0": lax.rem(zm, 2)}
    partner = {"tp": 1 - tp}

    def unit(u):
        return narrow if u == NARROW else wide.at[u if u < NARROW else u - 1]

    barrier = pltpu.get_barrier_semaphore()
    for other in (to_xp, to_xm, to_yp, to_ym, to_zp, to_zm, partner):
        pl.semaphore_signal(barrier, inc=1, device_id=other, device_id_type=MESH)

    loads = {}
    for n, (name, source, target) in enumerate((
        ("gate", gate_hbm, gate_w), ("up", up_hbm, up_w), ("down", down_hbm, down_w),
        ("v", v_hbm, v_w), ("u", u_hbm, u_w), ("out", out_hbm, out_w),
        ("tokens", tokens, whole.at[tp]),
    )):
        loads[name] = pltpu.make_async_copy(source, target, load_sem.at[n])
        loads[name].start()
    loaded = set()

    def need(*names):
        for name in names:
            if name not in loaded:
                loaded.add(name)
                loads[name].wait()

    diagonal = lax.broadcasted_iota(jnp.int32, (64, 64), 0) == lax.broadcasted_iota(
        jnp.int32, (64, 64), 1)

    def upright(ref):
        return jnp.sum(jnp.where(diagonal, ref[...], 0.0), axis=1, keepdims=True)

    def place(u):
        if u < 11:
            need("gate", "up")
            cols, row = slice(128 * u, 128 * u + 128), slice(u, u + 1)
            wide[u, z, y, x] = jnp.concatenate(
                [gate_w[:, cols] * gate_s[row], up_w[:, cols] * up_s[row]], axis=1).astype(BF)
        elif u < NARROW:
            need("down")
            at = 256 * (u - 11)
            wide[u, z, y, x] = (down_w[:, at : at + 256] * upright(down_s)).astype(BF)
        elif u == NARROW:
            need("down")
            narrow[z, y, x] = (down_w[:, 1280:1408] * upright(down_s)).astype(BF)
        else:
            at = 256 * ((u - 17) % 2)
            cols = slice(at, at + 256)
            if u < 19:
                need("v")
                value = v_w[:, cols] * v_s[:, cols]
            elif u < 21:
                need("u")
                value = u_w[:, cols] * u_s[:, cols]
            else:
                need("out")
                value = out_w[:, cols] * upright(out_s)
            wide[u - 1, z, y, x] = value.astype(BF)

    to_place = [code // 10 for code in PROGRAM if code < 1000 and code % 10 == 0]
    for _ in range(PLACED_AHEAD):
        place(to_place.pop(0))
    pl.semaphore_wait(barrier, 7)

    def send(ref, to, u, k):
        pltpu.make_async_remote_copy(
            src_ref=ref, dst_ref=ref, send_sem=sent.at[u, k], recv_sem=arrived.at[u, k],
            device_id=to, device_id_type=MESH,
        ).start()

    def region(u, k):
        b = unit(u)
        if ROUTES[u] < 2:
            return (b.at[0, 0, 0:2], b.at[0, 0, 0], b.at[0, 0:2], b.at[0, 0], b.at[0])[k]
        if ROUTES[u] < 4:
            return (b.at[0, 0, 0], b.at[0, 0], b.at[0, 0, 0:2], b.at[0], b.at[0, 0:2])[k]
        return (b.at[0, 0, 0:2], b.at[0, 0, 0], b.at[0, 0], b.at[0], b.at[0, 0:2])[k]

    def wait_for(u, k, sems):
        ref = region(u, k)
        pltpu.make_async_copy(ref, ref, sems.at[u, k]).wait()

    def step(u, k):
        if k > 0:
            wait_for(u, k - 1, arrived)
        elif to_place:
            place(to_place.pop(0))
        b, route = unit(u), ROUTES[u]
        if k == 5:
            return
        if route == 0:
            refs = (
                ((b.at[z, y, x], to_xp), (b.at[z, y, x], to_xm)),
                ((b.at[z, y, xm, 0:32], to_xp), (b.at[z, y, xp, 32:64], to_xm)),
                ((b.at[z, y], to_yp), (b.at[z, y], to_ym)),
                ((b.at[z, ym, 0:2], to_yp), (b.at[z, yp, 2:4], to_ym)),
                ((b.at[z, 0:2], to_zp), (b.at[z, 2:4], to_zm)),
            )
        elif route == 1:
            refs = (
                ((b.at[z, y, x], to_yp), (b.at[z, y, x], to_ym)),
                ((b.at[z, ym, x, 0:32], to_yp), (b.at[z, yp, x, 32:64], to_ym)),
                ((b.at[z, :, x], to_xp), (b.at[z, :, x], to_xm)),
                ((b.at[z, 0:2, xm], to_xp), (b.at[z, 2:4, xp], to_xm)),
                ((b.at[z, 0:2], to_zp), (b.at[z, 2:4], to_zm)),
            )
        elif route == 2:
            refs = (
                ((b.at[z, y, x, 0:32], to_zp), (b.at[z, y, x, 32:64], to_zm)),
                ((b.at[:, y, x], to_xp), (b.at[:, y, x], to_xm)),
                ((b.at[0, y, xm], to_xp), (b.at[1, y, xp], to_xm)),
                ((b.at[:, y], to_yp), (b.at[:, y], to_ym)),
                ((b.at[0, ym], to_yp), (b.at[1, yp], to_ym)),
            )
        elif route == 3:
            refs = (
                ((b.at[z, y, x, 0:32], to_zp), (b.at[z, y, x, 32:64], to_zm)),
                ((b.at[:, y, x], to_yp), (b.at[:, y, x], to_ym)),
                ((b.at[0, ym, x], to_yp), (b.at[1, yp, x], to_ym)),
                ((b.at[:, :, x], to_xp), (b.at[:, :, x], to_xm)),
                ((b.at[0, :, xm], to_xp), (b.at[1, :, xp], to_xm)),
            )
        elif route == 4:
            refs = (
                ((b.at[z, y, x], to_xp), (b.at[z, y, x], to_xm)),
                ((b.at[z, y, xm, 0:32], to_xp), (b.at[z, y, xp, 32:64], to_xm)),
                ((b.at[z, y, 0:2], to_zp), (b.at[z, y, 2:4], to_zm)),
                ((b.at[:, y], to_yp), (b.at[:, y], to_ym)),
                ((b.at[0, ym], to_yp), (b.at[1, yp], to_ym)),
            )
        else:
            refs = (
                ((b.at[z, y, x], to_yp), (b.at[z, y, x], to_ym)),
                ((b.at[z, ym, x, 0:32], to_yp), (b.at[z, yp, x, 32:64], to_ym)),
                ((b.at[z, 0:2, x], to_zp), (b.at[z, 2:4, x], to_zm)),
                ((b.at[:, :, x], to_xp), (b.at[:, :, x], to_xm)),
                ((b.at[0, :, xm], to_xp), (b.at[1, :, xp], to_xm)),
            )
        for ref, to in refs[k]:
            send(ref, to, u, k)

    def pair(src, dst, n):
        return pltpu.make_async_remote_copy(
            src_ref=src, dst_ref=dst, send_sem=pair_sent.at[n], recv_sem=pair_arrived.at[n],
            device_id=partner, device_id_type=MESH,
        )

    def rows_of(h):
        at, size = GROUPS_OF_ROWS[h]
        return pl.ds(at, size)

    exchange_tokens = pair(tokens, whole.at[tp], 0)
    exchange_tokens.start()
    exchange_first = [pair(part.at[rows_of(h)], got_first.at[rows_of(h)], 1 + h) for h in (0, 1)]
    exchange_stats = [pair(stats.at[rows_of(h)], stats_got.at[rows_of(h)], 3 + h) for h in (0, 1)]
    exchange_mix = [pair(part.at[rows_of(h)], got_mix.at[rows_of(h)], 5 + h) for h in (0, 1)]
    exchange_last = [
        pair(last_part.at[rows_of(h)], got_last.at[rows_of(h)], 7 + h) for h in (0, 1)
    ]

    stores = [
        pltpu.make_async_copy(last_part.at[rows_of(h)], result.at[rows_of(h)], store_sem.at[h])
        for h in (0, 1)
    ]

    def by_rows(at, size, step_rows, body):
        def one(i, carry):
            body(pl.ds(pl.multiple_of(at + i * step_rows, step_rows), step_rows))
            return carry

        lax.fori_loop(0, size // step_rows, one, 0, unroll=UNROLL if step_rows < SPAN else 1)

    def normalise(values, gain):
        factor = lax.rsqrt(jnp.mean(values * values, axis=1, keepdims=True) + EPS)
        return (values * factor * gain[...]).astype(BF)

    def norm_tokens():
        need("tokens")
        exchange_tokens.wait()

        def body(r):
            values = jnp.concatenate([whole[0, r], whole[1, r]], axis=1).astype(F32)
            normed[r] = normalise(values, norm_first)

        by_rows(0, 640, STEP_ROWS, body)

    def activate(both):
        return (silu(both[:, :128]) * both[:, 128:]).astype(BF)

    def first_hidden(u):
        for r in (pl.ds(0, 320), pl.ds(320, 320)):
            hidden[u, r] = activate(dot(normed[r], wide[u].reshape(2048, 256)))

    def down_rows(h, zi, yi):
        r = rows_of(h)
        left = jnp.concatenate([hidden[i, r] for i in range(11)], axis=1)
        right = jnp.concatenate(
            [wide[11 + j, zi, pl.ds(yi, 2)].reshape(512, 256) for j in range(5)]
            + [narrow[zi, pl.ds(yi, 2)].reshape(512, 128)], axis=1)
        return dot_t(left, right)

    def first_down(h, nb):
        part[rows_of(h), 512 * nb : 512 * nb + 512] = down_rows(h, nb // 2, 2 * (nb % 2)).astype(BF)
        if nb == 3:
            exchange_first[h].start()

    def combine_first(h):
        exchange_first[h].wait()

        def body(r):
            values = jnp.concatenate([whole[0, r], whole[1, r]], axis=1).astype(F32)
            branch = part[r].astype(F32) + got_first[r].astype(F32)
            total = (values + 0.5 * branch).astype(BF)
            middle[r] = total
            normed[r] = normalise(total.astype(F32), norm_mix)

        by_rows(*GROUPS_OF_ROWS[h], STEP_ROWS, body)

    def project_v(h):
        r = rows_of(h)
        lane = lax.broadcasted_iota(jnp.int32, (GROUPS_OF_ROWS[h][1], 128), 1)
        total = total_sq = 0.0
        for j in range(2):
            act = gelu(dot(normed[r], wide[16 + j].reshape(2048, 256)))
            v_act[r, 256 * j : 256 * j + 256] = act
            total += jnp.sum(act, axis=1, keepdims=True)
            total_sq += jnp.sum(act * act, axis=1, keepdims=True)
        stats[r] = jnp.where(lane == 0, total, jnp.where(lane == 1, total_sq, 0.0))
        exchange_stats[h].start()

    def project_u(h):
        r = rows_of(h)
        for j in range(2):
            act = gelu(dot(normed[r], wide[18 + j].reshape(2048, 256)))
            u_act[r, 256 * j : 256 * j + 256] = act

    def mix(h):
        exchange_stats[h].wait()
        row = lax.broadcasted_iota(jnp.int32, (SPAN, SPAN), 0)
        col = lax.broadcasted_iota(jnp.int32, (SPAN, SPAN), 1)

        def body(r):
            sums = stats[r] + stats_got[r]
            mean = sums[:, 0:1] * (1.0 / BW)
            var = sums[:, 1:2] * (1.0 / BW) - mean * mean
            factor = lax.rsqrt(var + EPS)
            for g in range(4):
                c = slice(128 * g, 128 * g + 128)
                v = ((v_act[r, c] - mean) * factor * ln_gain[:, c] + ln_bias[:, c]).astype(BF)
                w = jnp.where(col <= row, spatial_w[g].astype(F32), 0.0).astype(BF)
                bias = jnp.sum(
                    jnp.where(col == row, spatial_b[g : g + 1, :], 0.0), axis=1, keepdims=True)
                spatial = dot(w, v) + bias
                mixed[r, c] = (u_act[r, c] * spatial).astype(BF)

        by_rows(*GROUPS_OF_ROWS[h], SPAN, body)

    def project_out(h):
        r = rows_of(h)

        for nb in range(4):
            right = jnp.concatenate(
                [wide[20 + j, nb // 2, pl.ds(2 * (nb % 2), 2)].reshape(512, 256) for j in range(2)],
                axis=1)
            part[r, 512 * nb : 512 * nb + 512] = dot_t(mixed[r], right).astype(BF)
        exchange_mix[h].start()

    def combine_mix(h):
        exchange_mix[h].wait()

        def body(r):
            branch = part[r].astype(F32) + got_mix[r].astype(F32)
            total = (middle[r].astype(F32) + branch).astype(BF)
            middle[r] = total
            normed[r] = normalise(total.astype(F32), norm_second)

        by_rows(*GROUPS_OF_ROWS[h], STEP_ROWS, body)

    def second_hidden(h):
        r = rows_of(h)

        def product(u):
            return dot(normed[r], wide[u].reshape(2048, 256))

        for u in range(11):
            hidden[u, r] = activate(product(u))

    def second_down(h):
        r = rows_of(h)
        for nb in range(2):
            c = slice(512 * nb, 512 * nb + 512)
            last_part[r, c] = down_rows(h, 1 - tp, 2 * nb).astype(BF)
        exchange_last[h].start()
        for nb in range(2):
            c = slice(512 * nb, 512 * nb + 512)
            part[r, c] = down_rows(h, tp, 2 * nb).astype(BF)

    def finish(h):
        exchange_last[h].wait()

        def body(r):
            own = middle[r, pl.ds(pl.multiple_of(tp * 1024, 1024), 1024)].astype(F32)
            branch = part[r, 0:1024].astype(F32) + got_last[r].astype(F32)
            last_part[r] = (own + 0.5 * branch).astype(BF)

        by_rows(*GROUPS_OF_ROWS[h], STEP_ROWS, body)
        stores[h].start()

    def task(n):
        if n == 90:
            norm_tokens()
        elif n < 120:
            first_hidden(n - 100)
        elif n < 130:
            first_down((n - 120) // 4, n % 4)
        else:
            run = (combine_first, project_v, project_u, mix, project_out)
            run[n // 10 - 13](n % 10)

    for code in PROGRAM:
        if code < 1000:
            step(code // 10, code % 10)
        else:
            task(code - 1000)
    for h in (0, 1):
        combine_mix(h)
        second_hidden(h)
        second_down(h)
    for h in (0, 1):
        finish(h)
    for u in range(N_UNITS):
        for k in range(5):
            wait_for(u, k, sent)
    for store in stores:
        store.wait()


def on_device(*args):
    (tokens, norm_first, norm_mix, norm_second, gate_w, up_w, down_w, gate_s, up_s, down_s,
     u_w, v_w, u_s, v_s, ln_gain, ln_bias, spatial_w, spatial_b, out_w, out_s) = args
    line = lambda a: a.reshape(1, -1)
    rows = tokens.shape[0]
    vmem = pltpu.VMEM
    return pl.pallas_call(
        kernel,
        out_shape=jax.ShapeDtypeStruct(tokens.shape, BF),
        in_specs=[
            pl.BlockSpec(memory_space=pl.ANY if n in (0, 4, 5, 6, 10, 11, 18) else pltpu.VMEM)
            for n in range(20)
        ],
        out_specs=pl.BlockSpec(memory_space=pl.ANY),
        scratch_shapes=[
            *[vmem((64, 1408), F32)] * 3,
            *[vmem((64, 512), F32)] * 3,
            vmem((N_UNITS - 1, 2, 4, 4, 64, 256), BF),
            vmem((2, 4, 4, 64, 128), BF),
            vmem((2, rows, 1024), BF),
            vmem((rows, 2048), BF),
            vmem((rows, 2048), BF),
            vmem((11, rows, 128), BF),
            vmem((rows, 2048), BF),
            vmem((rows, 2048), BF),
            vmem((rows, 2048), BF),
            vmem((rows, 1024), BF),
            vmem((rows, 1024), BF),
            vmem((rows, 512), F32),
            vmem((rows, 512), F32),
            vmem((rows, 512), BF),
            vmem((rows, 128), F32),
            vmem((rows, 128), F32),
            pltpu.SemaphoreType.DMA((N_UNITS, 5)),
            pltpu.SemaphoreType.DMA((N_UNITS, 5)),
            *[pltpu.SemaphoreType.DMA((n,)) for n in (9, 9, 7, 2)],
        ],
        compiler_params=pltpu.CompilerParams(
            collective_id=0, has_side_effects=True, vmem_limit_bytes=67043328
        ),
    )(tokens, line(norm_first), line(norm_mix), line(norm_second), gate_w, up_w, down_w.T,
      gate_s.reshape(-1, 128), up_s.reshape(-1, 128), line(down_s), u_w, v_w, line(u_s), line(v_s), line(ln_gain),
      line(ln_bias), spatial_w, spatial_b, out_w.T, line(out_s))


def solution(mesh):
    torus = Mesh(
        mesh.devices.reshape(mesh.shape["rep"], 2, 4, 4, mesh.shape["tp"]),
        ("rep", "fs_0", "fs_1", "fs_2", "tp"),
    )
    in_specs = (
        P(REP_FS, "tp"), P(), P(), P(), P(FS, "tp"), P(FS, "tp"), P("tp", FS), P("tp"), P("tp"),
        P(FS), P(FS, "tp"), P(FS, "tp"), P("tp"), P("tp"), P("tp"), P("tp"),
        P("tp", None, None), P("tp", None), P("tp", FS), P(FS),
    )
    return jax.shard_map(
        on_device, mesh=torus, in_specs=in_specs, out_specs=P(REP_FS, "tp"), check_vma=False
    )
```

```python
import functools

import jax
import jax.numpy as jnp
from jax import lax
from jax.experimental import pallas as pl
from jax.experimental.pallas import tpu as pltpu
from jax.sharding import Mesh
from jax.sharding import PartitionSpec as P

BW = 1024
SPAN = 128
EPS = 1e-06
FS = ("fs_0", "fs_1", "fs_2")
REP_FS = ("rep", "fs_0", "fs_1", "fs_2")
MESH = pl.DeviceIdType.MESH
BF = jnp.bfloat16
F32 = jnp.float32

N_UNITS = 23
NARROW = 16
ROUTES = (
    0, 0, 4, 1, 5, 5, 1, 2, 1, 0, 1, 4, 1, 4, 4, 5, 0, 1, 1, 2, 3, 5, 2,
)
PROGRAM = (
    60, 90, 100, 150, 0, 40, 160, 130, 61, 80, 91, 50, 101, 20, 10, 151, 1, 140, 161, 120, 41,
    1090, 62, 92, 131, 81, 51, 21, 102, 30, 11, 152, 70, 2, 170, 121, 110, 141, 162, 42, 153, 71,
    63, 93, 132, 82, 22, 52, 43, 31, 103, 133, 12, 3, 111, 142, 171, 23, 122, 53, 163, 94, 143,
    32, 154, 72, 64, 134, 95, 180, 1109, 83, 13, 4, 172, 65, 190, 1106, 44, 104, 112, 24, 164,
    123, 5, 220, 1100, 191, 144, 54, 105, 210, 1110, 135, 200, 181, 113, 33, 14, 165, 155, 221,
    201, 73, 25, 1102, 84, 145, 211, 182, 173, 15, 1101, 45, 1104, 124, 114, 192, 85, 1108, 202,
    55, 1105, 34, 222, 125, 74, 212, 183, 174, 115, 193, 203, 223, 35, 1103, 184, 75, 1107, 213,
    1120, 1121, 1122, 1123, 1124, 1125, 1126, 204, 1127, 194, 175, 1130, 1131, 214, 224, 185,
    1140, 1141, 205, 195, 1150, 1151, 1160, 215, 1161, 225, 1170, 1171,
)

GROUPS_OF_ROWS = ((0, 384), (384, 256))
STEP_ROWS = 16
UNROLL = 8
PLACED_AHEAD = 4


def gelu(a):
    return 0.5 * a * (1.0 + jnp.tanh(0.7978845608028654 * (a + 0.044715 * (a * a * a))))


def silu(a):
    return 0.5 * a * (1.0 + jnp.tanh(0.5 * a))


def dot(a, b):
    return jnp.dot(a, b, preferred_element_type=F32)


def dot_t(a, b):
    return lax.dot_general(a, b, (((1,), (1,)), ((), ())), preferred_element_type=F32)


def kernel(
    tokens, norm_first_hbm, norm_mix_hbm, norm_second_hbm, gate_hbm, up_hbm, down_hbm,
    gate_s_hbm, up_s_hbm, down_s_hbm, u_hbm, v_hbm, u_s_hbm, v_s_hbm, ln_gain_hbm, ln_bias_hbm,
    spatial_w_hbm, spatial_b_hbm, out_hbm, out_s_hbm,
    result,
    norm_first, norm_mix, norm_second, gate_s, up_s, down_s, u_s, v_s, ln_gain, ln_bias,
    spatial_w, spatial_b, out_s,
    gate_w, up_w, down_w, v_w, u_w, out_w,
    wide, narrow, whole, normed, middle, hidden, part, got_first, got_mix, last_part, got_last,
    u_act, v_act, mixed, stats, stats_got,
    sent, arrived, pair_sent, pair_arrived, load_sem, store_sem,
):
    rep, z, y, x, tp = (lax.axis_index(a) for a in ("rep", "fs_0", "fs_1", "fs_2", "tp"))
    xp, xm = lax.rem(x + 1, 4), lax.rem(x + 3, 4)
    yp, ym = lax.rem(y + 1, 4), lax.rem(y + 3, 4)
    full_z = rep * 2 + z
    zp, zm = lax.rem(full_z + 1, 4), lax.rem(full_z + 3, 4)
    to_xp, to_xm = {"fs_2": xp}, {"fs_2": xm}
    to_yp, to_ym = {"fs_1": yp}, {"fs_1": ym}
    to_zp = {"rep": zp // 2, "fs_0": lax.rem(zp, 2)}
    to_zm = {"rep": zm // 2, "fs_0": lax.rem(zm, 2)}
    partner = {"tp": 1 - tp}

    def unit(u):
        return narrow if u == NARROW else wide.at[u if u < NARROW else u - 1]

    barrier = pltpu.get_barrier_semaphore()
    for other in (to_xp, to_xm, to_yp, to_ym, to_zp, to_zm, partner):
        pl.semaphore_signal(barrier, inc=1, device_id=other, device_id_type=MESH)

    loads = {}
    for n, (name, source, target) in enumerate((
        ("gate_s", gate_s_hbm, gate_s), ("up_s", up_s_hbm, up_s), ("down_s", down_s_hbm, down_s),
        ("gate", gate_hbm, gate_w), ("up", up_hbm, up_w), ("down", down_hbm, down_w),
        ("v_s", v_s_hbm, v_s), ("u_s", u_s_hbm, u_s), ("out_s", out_s_hbm, out_s),
        ("v", v_hbm, v_w), ("u", u_hbm, u_w), ("out", out_hbm, out_w),
        ("first", norm_first_hbm, norm_first), ("tokens", tokens, whole.at[tp]),
        ("mix", norm_mix_hbm, norm_mix), ("second", norm_second_hbm, norm_second),
        ("gain", ln_gain_hbm, ln_gain), ("bias", ln_bias_hbm, ln_bias),
        ("spatial_w", spatial_w_hbm, spatial_w), ("spatial_b", spatial_b_hbm, spatial_b),
    )):
        loads[name] = pltpu.make_async_copy(source, target, load_sem.at[n])
        loads[name].start()
    loaded = set()

    def need(*names):
        for name in names:
            if name not in loaded:
                loaded.add(name)
                loads[name].wait()

    diagonal = lax.broadcasted_iota(jnp.int32, (64, 64), 0) == lax.broadcasted_iota(
        jnp.int32, (64, 64), 1)

    def upright(ref):
        return jnp.sum(jnp.where(diagonal, ref[...], 0.0), axis=1, keepdims=True)

    def place(u):
        if u < 11:
            need("gate", "up", "gate_s", "up_s")
            cols, row = slice(128 * u, 128 * u + 128), slice(u, u + 1)
            wide[u, z, y, x] = jnp.concatenate(
                [gate_w[:, cols] * gate_s[row], up_w[:, cols] * up_s[row]], axis=1).astype(BF)
        elif u < NARROW:
            need("down", "down_s")
            at = 256 * (u - 11)
            wide[u, z, y, x] = (down_w[:, at : at + 256] * upright(down_s)).astype(BF)
        elif u == NARROW:
            need("down", "down_s")
            narrow[z, y, x] = (down_w[:, 1280:1408] * upright(down_s)).astype(BF)
        else:
            at = 256 * ((u - 17) % 2)
            cols = slice(at, at + 256)
            if u < 19:
                need("v", "v_s")
                value = v_w[:, cols] * v_s[:, cols]
            elif u < 21:
                need("u", "u_s")
                value = u_w[:, cols] * u_s[:, cols]
            else:
                need("out", "out_s")
                value = out_w[:, cols] * upright(out_s)
            wide[u - 1, z, y, x] = value.astype(BF)

    to_place = [code // 10 for code in PROGRAM if code < 1000 and code % 10 == 0]
    for _ in range(PLACED_AHEAD):
        place(to_place.pop(0))
    pl.semaphore_wait(barrier, 7)

    def send(ref, to, u, k):
        pltpu.make_async_remote_copy(
            src_ref=ref, dst_ref=ref, send_sem=sent.at[u, k], recv_sem=arrived.at[u, k],
            device_id=to, device_id_type=MESH,
        ).start()

    def region(u, k):
        b = unit(u)
        if ROUTES[u] < 2:
            return (b.at[0, 0, 0:2], b.at[0, 0, 0], b.at[0, 0:2], b.at[0, 0], b.at[0])[k]
        if ROUTES[u] < 4:
            return (b.at[0, 0, 0], b.at[0, 0], b.at[0, 0, 0:2], b.at[0], b.at[0, 0:2])[k]
        return (b.at[0, 0, 0:2], b.at[0, 0, 0], b.at[0, 0], b.at[0], b.at[0, 0:2])[k]

    def wait_for(u, k, sems):
        ref = region(u, k)
        pltpu.make_async_copy(ref, ref, sems.at[u, k]).wait()

    def step(u, k):
        if k > 0:
            wait_for(u, k - 1, arrived)
        elif to_place:
            place(to_place.pop(0))
        b, route = unit(u), ROUTES[u]
        if k == 5:
            return
        if route == 0:
            refs = (
                ((b.at[z, y, x], to_xp), (b.at[z, y, x], to_xm)),
                ((b.at[z, y, xm, 0:32], to_xp), (b.at[z, y, xp, 32:64], to_xm)),
                ((b.at[z, y], to_yp), (b.at[z, y], to_ym)),
                ((b.at[z, ym, 0:2], to_yp), (b.at[z, yp, 2:4], to_ym)),
                ((b.at[z, 0:2], to_zp), (b.at[z, 2:4], to_zm)),
            )
        elif route == 1:
            refs = (
                ((b.at[z, y, x], to_yp), (b.at[z, y, x], to_ym)),
                ((b.at[z, ym, x, 0:32], to_yp), (b.at[z, yp, x, 32:64], to_ym)),
                ((b.at[z, :, x], to_xp), (b.at[z, :, x], to_xm)),
                ((b.at[z, 0:2, xm], to_xp), (b.at[z, 2:4, xp], to_xm)),
                ((b.at[z, 0:2], to_zp), (b.at[z, 2:4], to_zm)),
            )
        elif route == 2:
            refs = (
                ((b.at[z, y, x, 0:32], to_zp), (b.at[z, y, x, 32:64], to_zm)),
                ((b.at[:, y, x], to_xp), (b.at[:, y, x], to_xm)),
                ((b.at[0, y, xm], to_xp), (b.at[1, y, xp], to_xm)),
                ((b.at[:, y], to_yp), (b.at[:, y], to_ym)),
                ((b.at[0, ym], to_yp), (b.at[1, yp], to_ym)),
            )
        elif route == 3:
            refs = (
                ((b.at[z, y, x, 0:32], to_zp), (b.at[z, y, x, 32:64], to_zm)),
                ((b.at[:, y, x], to_yp), (b.at[:, y, x], to_ym)),
                ((b.at[0, ym, x], to_yp), (b.at[1, yp, x], to_ym)),
                ((b.at[:, :, x], to_xp), (b.at[:, :, x], to_xm)),
                ((b.at[0, :, xm], to_xp), (b.at[1, :, xp], to_xm)),
            )
        elif route == 4:
            refs = (
                ((b.at[z, y, x], to_xp), (b.at[z, y, x], to_xm)),
                ((b.at[z, y, xm, 0:32], to_xp), (b.at[z, y, xp, 32:64], to_xm)),
                ((b.at[z, y, 0:2], to_zp), (b.at[z, y, 2:4], to_zm)),
                ((b.at[:, y], to_yp), (b.at[:, y], to_ym)),
                ((b.at[0, ym], to_yp), (b.at[1, yp], to_ym)),
            )
        else:
            refs = (
                ((b.at[z, y, x], to_yp), (b.at[z, y, x], to_ym)),
                ((b.at[z, ym, x, 0:32], to_yp), (b.at[z, yp, x, 32:64], to_ym)),
                ((b.at[z, 0:2, x], to_zp), (b.at[z, 2:4, x], to_zm)),
                ((b.at[:, :, x], to_xp), (b.at[:, :, x], to_xm)),
                ((b.at[0, :, xm], to_xp), (b.at[1, :, xp], to_xm)),
            )
        for ref, to in refs[k]:
            send(ref, to, u, k)

    def pair(src, dst, n):
        return pltpu.make_async_remote_copy(
            src_ref=src, dst_ref=dst, send_sem=pair_sent.at[n], recv_sem=pair_arrived.at[n],
            device_id=partner, device_id_type=MESH,
        )

    def columns(n):
        return [pl.ds(512 * i, 512) for i in range(n)]

    def rows_of(h):
        at, size = GROUPS_OF_ROWS[h]
        return pl.ds(at, size)

    exchange_tokens = pair(tokens, whole.at[tp], 0)
    exchange_tokens.start()
    exchange_first = [pair(part.at[rows_of(h)], got_first.at[rows_of(h)], 1 + h) for h in (0, 1)]
    exchange_stats = [pair(stats.at[rows_of(h)], stats_got.at[rows_of(h)], 3 + h) for h in (0, 1)]
    exchange_mix = [
        [pair(part.at[rows_of(h), c], got_mix.at[rows_of(h), c], 5 + 4 * h + i)
         for i, c in enumerate(columns(4))] for h in (0, 1)
    ]
    exchange_last = [
        [pair(last_part.at[rows_of(h), c], got_last.at[rows_of(h), c], 13 + 2 * h + i)
         for i, c in enumerate(columns(2))] for h in (0, 1)
    ]

    stores = [
        pltpu.make_async_copy(last_part.at[rows_of(h)], result.at[rows_of(h)], store_sem.at[h])
        for h in (0, 1)
    ]

    def by_rows(at, size, step_rows, body):
        def one(i, carry):
            body(pl.ds(pl.multiple_of(at + i * step_rows, step_rows), step_rows))
            return carry

        lax.fori_loop(0, size // step_rows, one, 0, unroll=UNROLL if step_rows < SPAN else 1)

    def normalise(values, gain):
        factor = lax.rsqrt(jnp.mean(values * values, axis=1, keepdims=True) + EPS)
        return (values * factor * gain[...]).astype(BF)

    def norm_tokens():
        need("tokens", "first", "mix", "second", "gain", "bias", "spatial_w", "spatial_b")
        exchange_tokens.wait()

        def body(r):
            values = jnp.concatenate([whole[0, r], whole[1, r]], axis=1).astype(F32)
            normed[r] = normalise(values, norm_first)

        by_rows(0, 640, STEP_ROWS, body)

    def activate(both):
        return (silu(both[:, :128]) * both[:, 128:]).astype(BF)

    def first_hidden(u):
        for r in (pl.ds(0, 320), pl.ds(320, 320)):
            hidden[u, r] = activate(dot(normed[r], wide[u].reshape(2048, 256)))

    def down_rows(h, zi, yi):
        r = rows_of(h)
        left = jnp.concatenate([hidden[i, r] for i in range(11)], axis=1)
        right = jnp.concatenate(
            [wide[11 + j, zi, pl.ds(yi, 2)].reshape(512, 256) for j in range(5)]
            + [narrow[zi, pl.ds(yi, 2)].reshape(512, 128)], axis=1)
        return dot_t(left, right)

    def first_down(h, nb):
        part[rows_of(h), 512 * nb : 512 * nb + 512] = down_rows(h, nb // 2, 2 * (nb % 2)).astype(BF)
        if nb == 3:
            exchange_first[h].start()

    def combine_first(h):
        exchange_first[h].wait()

        def body(r):
            values = jnp.concatenate([whole[0, r], whole[1, r]], axis=1).astype(F32)
            branch = part[r].astype(F32) + got_first[r].astype(F32)
            total = (values + 0.5 * branch).astype(BF)
            middle[r] = total
            normed[r] = normalise(total.astype(F32), norm_mix)

        by_rows(*GROUPS_OF_ROWS[h], STEP_ROWS, body)

    def project_v(h):
        r = rows_of(h)
        lane = lax.broadcasted_iota(jnp.int32, (GROUPS_OF_ROWS[h][1], 128), 1)
        total = total_sq = 0.0
        for j in range(2):
            act = gelu(dot(normed[r], wide[16 + j].reshape(2048, 256)))
            v_act[r, 256 * j : 256 * j + 256] = act
            total += jnp.sum(act, axis=1, keepdims=True)
            total_sq += jnp.sum(act * act, axis=1, keepdims=True)
        stats[r] = jnp.where(lane == 0, total, jnp.where(lane == 1, total_sq, 0.0))
        exchange_stats[h].start()

    def project_u(h):
        r = rows_of(h)
        for j in range(2):
            act = gelu(dot(normed[r], wide[18 + j].reshape(2048, 256)))
            u_act[r, 256 * j : 256 * j + 256] = act

    def mix(h):
        exchange_stats[h].wait()
        row = lax.broadcasted_iota(jnp.int32, (SPAN, SPAN), 0)
        col = lax.broadcasted_iota(jnp.int32, (SPAN, SPAN), 1)

        def body(r):
            sums = stats[r] + stats_got[r]
            mean = sums[:, 0:1] * (1.0 / BW)
            var = sums[:, 1:2] * (1.0 / BW) - mean * mean
            factor = lax.rsqrt(var + EPS)
            for g in range(4):
                c = slice(128 * g, 128 * g + 128)
                v = ((v_act[r, c] - mean) * factor * ln_gain[:, c] + ln_bias[:, c]).astype(BF)
                w = jnp.where(col <= row, spatial_w[g].astype(F32), 0.0).astype(BF)
                bias = jnp.sum(
                    jnp.where(col == row, spatial_b[g : g + 1, :], 0.0), axis=1, keepdims=True)
                spatial = dot(w, v) + bias
                mixed[r, c] = (u_act[r, c] * spatial).astype(BF)

        by_rows(*GROUPS_OF_ROWS[h], SPAN, body)

    def project_out(h):
        r = rows_of(h)

        for nb in range(4):
            right = jnp.concatenate(
                [wide[20 + j, nb // 2, pl.ds(2 * (nb % 2), 2)].reshape(512, 256) for j in range(2)],
                axis=1)
            part[r, 512 * nb : 512 * nb + 512] = dot_t(mixed[r], right).astype(BF)
            if nb:
                exchange_mix[h][nb - 1].start()
        exchange_mix[h][3].start()

    def combine_mix(h):
        for block in exchange_mix[h]:
            block.wait()

        def body(r):
            branch = part[r].astype(F32) + got_mix[r].astype(F32)
            total = (middle[r].astype(F32) + branch).astype(BF)
            middle[r] = total
            normed[r] = normalise(total.astype(F32), norm_second)

        by_rows(*GROUPS_OF_ROWS[h], STEP_ROWS, body)

    def second_hidden(h):
        r = rows_of(h)

        def product(u):
            return dot(normed[r], wide[u].reshape(2048, 256))

        for u in range(11):
            hidden[u, r] = activate(product(u))

    def second_down(h):
        r = rows_of(h)
        for nb in range(2):
            c = slice(512 * nb, 512 * nb + 512)
            last_part[r, c] = down_rows(h, 1 - tp, 2 * nb).astype(BF)
            if nb:
                exchange_last[h][0].start()
        exchange_last[h][1].start()
        for nb in range(2):
            c = slice(512 * nb, 512 * nb + 512)
            part[r, c] = down_rows(h, tp, 2 * nb).astype(BF)

    def finish(h):
        for block in exchange_last[h]:
            block.wait()

        def body(r):
            own = middle[r, pl.ds(pl.multiple_of(tp * 1024, 1024), 1024)].astype(F32)
            branch = part[r, 0:1024].astype(F32) + got_last[r].astype(F32)
            last_part[r] = (own + 0.5 * branch).astype(BF)

        by_rows(*GROUPS_OF_ROWS[h], STEP_ROWS, body)
        stores[h].start()

    def task(n):
        if n == 90:
            norm_tokens()
        elif n < 120:
            first_hidden(n - 100)
        elif n < 130:
            first_down((n - 120) // 4, n % 4)
        else:
            run = (combine_first, project_v, project_u, mix, project_out)
            run[n // 10 - 13](n % 10)

    for code in PROGRAM:
        if code < 1000:
            step(code // 10, code % 10)
        else:
            task(code - 1000)
    for h in (0, 1):
        combine_mix(h)
        second_hidden(h)
        second_down(h)
    for h in (0, 1):
        finish(h)
    for u in range(N_UNITS):
        for k in range(5):
            wait_for(u, k, sent)
    for store in stores:
        store.wait()


def on_device(*args):
    (tokens, norm_first, norm_mix, norm_second, gate_w, up_w, down_w, gate_s, up_s, down_s,
     u_w, v_w, u_s, v_s, ln_gain, ln_bias, spatial_w, spatial_b, out_w, out_s) = args
    line = lambda a: a.reshape(1, -1)
    rows = tokens.shape[0]
    vmem = pltpu.VMEM
    return pl.pallas_call(
        kernel,
        out_shape=jax.ShapeDtypeStruct(tokens.shape, BF),
        in_specs=[pl.BlockSpec(memory_space=pl.ANY)] * 20,
        out_specs=pl.BlockSpec(memory_space=pl.ANY),
        scratch_shapes=[
            *[vmem((1, 2048), F32)] * 3,
            *[vmem((11, 128), F32)] * 2,
            vmem((1, 64), F32),
            *[vmem((1, 512), F32)] * 4,
            vmem((4, 128, 128), BF),
            vmem((4, 128), F32),
            vmem((1, 64), F32),
            *[vmem((64, 1408), F32)] * 3,
            *[vmem((64, 512), F32)] * 3,
            vmem((N_UNITS - 1, 2, 4, 4, 64, 256), BF),
            vmem((2, 4, 4, 64, 128), BF),
            vmem((2, rows, 1024), BF),
            vmem((rows, 2048), BF),
            vmem((rows, 2048), BF),
            vmem((11, rows, 128), BF),
            vmem((rows, 2048), BF),
            vmem((rows, 2048), BF),
            vmem((rows, 2048), BF),
            vmem((rows, 1024), BF),
            vmem((rows, 1024), BF),
            vmem((rows, 512), F32),
            vmem((rows, 512), F32),
            vmem((rows, 512), BF),
            vmem((rows, 128), F32),
            vmem((rows, 128), F32),
            pltpu.SemaphoreType.DMA((N_UNITS, 5)),
            pltpu.SemaphoreType.DMA((N_UNITS, 5)),
            *[pltpu.SemaphoreType.DMA((n,)) for n in (17, 17, 20, 2)],
        ],
        compiler_params=pltpu.CompilerParams(
            collective_id=0, has_side_effects=True, vmem_limit_bytes=67043328
        ),
    )(tokens, line(norm_first), line(norm_mix), line(norm_second), gate_w, up_w, down_w.T,
      gate_s.reshape(-1, 128), up_s.reshape(-1, 128), line(down_s), u_w, v_w, line(u_s), line(v_s), line(ln_gain),
      line(ln_bias), spatial_w, spatial_b, out_w.T, line(out_s))


def solution(mesh):
    torus = Mesh(
        mesh.devices.reshape(mesh.shape["rep"], 2, 4, 4, mesh.shape["tp"]),
        ("rep", "fs_0", "fs_1", "fs_2", "tp"),
    )
    in_specs = (
        P(REP_FS, "tp"), P(), P(), P(), P(FS, "tp"), P(FS, "tp"), P("tp", FS), P("tp"), P("tp"),
        P(FS), P(FS, "tp"), P(FS, "tp"), P("tp"), P("tp"), P("tp"), P("tp"),
        P("tp", None, None), P("tp", None), P("tp", FS), P(FS),
    )
    return jax.shard_map(
        on_device, mesh=torus, in_specs=in_specs, out_specs=P(REP_FS, "tp"), check_vma=False
    )
```

```python
import functools

import jax
import jax.numpy as jnp
from jax import lax
from jax.experimental import pallas as pl
from jax.experimental.pallas import tpu as pltpu
from jax.sharding import Mesh
from jax.sharding import PartitionSpec as P

BW = 1024
SPAN = 128
EPS = 1e-06
FS = ("fs_0", "fs_1", "fs_2")
REP_FS = ("rep", "fs_0", "fs_1", "fs_2")
MESH = pl.DeviceIdType.MESH
BF = jnp.bfloat16
F32 = jnp.float32

N_UNITS = 23
NARROW = 16
ROUTES = (
    0, 0, 4, 1, 5, 5, 1, 2, 1, 0, 1, 4, 1, 4, 4, 5, 0, 1, 1, 2, 3, 5, 2,
)
PROGRAM = (
    60, 90, 100, 150, 0, 40, 160, 130, 61, 80, 91, 50, 101, 20, 10, 151, 1, 140, 161, 120, 41,
    1090, 62, 92, 131, 81, 51, 21, 102, 30, 11, 152, 70, 2, 170, 121, 110, 141, 162, 42, 153, 71,
    63, 93, 132, 82, 22, 52, 43, 31, 103, 133, 12, 3, 111, 142, 171, 23, 122, 53, 163, 94, 143,
    32, 154, 72, 64, 134, 95, 180, 1109, 83, 13, 4, 172, 65, 190, 1106, 44, 104, 112, 24, 164,
    123, 5, 220, 1100, 191, 144, 54, 105, 210, 1110, 135, 200, 181, 113, 33, 14, 165, 155, 221,
    201, 73, 25, 1102, 84, 145, 211, 182, 173, 15, 1101, 45, 1104, 124, 114, 192, 85, 1108, 202,
    55, 1105, 34, 222, 125, 74, 212, 183, 174, 115, 193, 203, 223, 35, 1103, 184, 75, 1107, 213,
    1120, 1121, 1122, 1123, 1124, 1125, 1126, 204, 1127, 194, 175, 1130, 1131, 214, 224, 185,
    1140, 1141, 205, 195, 1150, 1151, 1160, 215, 1161, 225, 1170, 1171,
)

GROUPS_OF_ROWS = ((0, 256), (256, 384))
STEP_ROWS = 16
UNROLL = 8
PLACED_AHEAD = 4


def gelu(a):
    return 0.5 * a * (1.0 + jnp.tanh(0.7978845608028654 * (a + 0.044715 * (a * a * a))))


def silu(a):
    return 0.5 * a * (1.0 + jnp.tanh(0.5 * a))


def dot(a, b):
    return jnp.dot(a, b, preferred_element_type=F32)


def dot_t(a, b):
    return lax.dot_general(a, b, (((1,), (1,)), ((), ())), preferred_element_type=F32)


def kernel(
    tokens, norm_first_hbm, norm_mix_hbm, norm_second_hbm, gate_hbm, up_hbm, down_hbm,
    gate_s_hbm, up_s_hbm, down_s_hbm, u_hbm, v_hbm, u_s_hbm, v_s_hbm, ln_gain_hbm, ln_bias_hbm,
    spatial_w_hbm, spatial_b_hbm, out_hbm, out_s_hbm,
    result,
    norm_first, norm_mix, norm_second, gate_s, up_s, down_s, u_s, v_s, ln_gain, ln_bias,
    spatial_w, spatial_b, out_s,
    gate_w, up_w, down_w, v_w, u_w, out_w,
    wide, narrow, whole, normed, middle, hidden, part, got_first, got_mix, last_part, got_last,
    u_act, v_act, mixed, stats, stats_got,
    sent, arrived, pair_sent, pair_arrived, load_sem, store_sem,
):
    rep, z, y, x, tp = (lax.axis_index(a) for a in ("rep", "fs_0", "fs_1", "fs_2", "tp"))
    xp, xm = lax.rem(x + 1, 4), lax.rem(x + 3, 4)
    yp, ym = lax.rem(y + 1, 4), lax.rem(y + 3, 4)
    full_z = rep * 2 + z
    zp, zm = lax.rem(full_z + 1, 4), lax.rem(full_z + 3, 4)
    to_xp, to_xm = {"fs_2": xp}, {"fs_2": xm}
    to_yp, to_ym = {"fs_1": yp}, {"fs_1": ym}
    to_zp = {"rep": zp // 2, "fs_0": lax.rem(zp, 2)}
    to_zm = {"rep": zm // 2, "fs_0": lax.rem(zm, 2)}
    partner = {"tp": 1 - tp}

    def unit(u):
        return narrow if u == NARROW else wide.at[u if u < NARROW else u - 1]

    barrier = pltpu.get_barrier_semaphore()
    for other in (to_xp, to_xm, to_yp, to_ym, to_zp, to_zm, partner):
        pl.semaphore_signal(barrier, inc=1, device_id=other, device_id_type=MESH)

    loads = {}
    for n, (name, source, target) in enumerate((
        ("gate_s", gate_s_hbm, gate_s), ("up_s", up_s_hbm, up_s), ("down_s", down_s_hbm, down_s),
        ("gate", gate_hbm, gate_w), ("up", up_hbm, up_w), ("down", down_hbm, down_w),
        ("v_s", v_s_hbm, v_s), ("u_s", u_s_hbm, u_s), ("out_s", out_s_hbm, out_s),
        ("v", v_hbm, v_w), ("u", u_hbm, u_w), ("out", out_hbm, out_w),
        ("first", norm_first_hbm, norm_first), ("tokens", tokens, whole.at[tp]),
        ("mix", norm_mix_hbm, norm_mix), ("second", norm_second_hbm, norm_second),
        ("gain", ln_gain_hbm, ln_gain), ("bias", ln_bias_hbm, ln_bias),
        ("spatial_w", spatial_w_hbm, spatial_w), ("spatial_b", spatial_b_hbm, spatial_b),
    )):
        loads[name] = pltpu.make_async_copy(source, target, load_sem.at[n])
        loads[name].start()
    loaded = set()

    def need(*names):
        for name in names:
            if name not in loaded:
                loaded.add(name)
                loads[name].wait()

    diagonal = lax.broadcasted_iota(jnp.int32, (64, 64), 0) == lax.broadcasted_iota(
        jnp.int32, (64, 64), 1)

    def upright(ref):
        return jnp.sum(jnp.where(diagonal, ref[...], 0.0), axis=1, keepdims=True)

    def place(u):
        if u < 11:
            need("gate", "up", "gate_s", "up_s")
            cols, row = slice(128 * u, 128 * u + 128), slice(u, u + 1)
            wide[u, z, y, x] = jnp.concatenate(
                [gate_w[:, cols] * gate_s[row], up_w[:, cols] * up_s[row]], axis=1).astype(BF)
        elif u < NARROW:
            need("down", "down_s")
            at = 256 * (u - 11)
            wide[u, z, y, x] = (down_w[:, at : at + 256] * upright(down_s)).astype(BF)
        elif u == NARROW:
            need("down", "down_s")
            narrow[z, y, x] = (down_w[:, 1280:1408] * upright(down_s)).astype(BF)
        else:
            at = 256 * ((u - 17) % 2)
            cols = slice(at, at + 256)
            if u < 19:
                need("v", "v_s")
                value = v_w[:, cols] * v_s[:, cols]
            elif u < 21:
                need("u", "u_s")
                value = u_w[:, cols] * u_s[:, cols]
            else:
                need("out", "out_s")
                value = out_w[:, cols] * upright(out_s)
            wide[u - 1, z, y, x] = value.astype(BF)

    to_place = [code // 10 for code in PROGRAM if code < 1000 and code % 10 == 0]
    for _ in range(PLACED_AHEAD):
        place(to_place.pop(0))
    pl.semaphore_wait(barrier, 7)

    def send(ref, to, u, k):
        pltpu.make_async_remote_copy(
            src_ref=ref, dst_ref=ref, send_sem=sent.at[u, k], recv_sem=arrived.at[u, k],
            device_id=to, device_id_type=MESH,
        ).start()

    def region(u, k):
        b = unit(u)
        if ROUTES[u] < 2:
            return (b.at[0, 0, 0:2], b.at[0, 0, 0], b.at[0, 0:2], b.at[0, 0], b.at[0])[k]
        if ROUTES[u] < 4:
            return (b.at[0, 0, 0], b.at[0, 0], b.at[0, 0, 0:2], b.at[0], b.at[0, 0:2])[k]
        return (b.at[0, 0, 0:2], b.at[0, 0, 0], b.at[0, 0], b.at[0], b.at[0, 0:2])[k]

    def wait_for(u, k, sems):
        ref = region(u, k)
        pltpu.make_async_copy(ref, ref, sems.at[u, k]).wait()

    def step(u, k):
        if k > 0:
            wait_for(u, k - 1, arrived)
        elif to_place:
            place(to_place.pop(0))
        b, route = unit(u), ROUTES[u]
        if k == 5:
            return
        if route == 0:
            refs = (
                ((b.at[z, y, x], to_xp), (b.at[z, y, x], to_xm)),
                ((b.at[z, y, xm, 0:32], to_xp), (b.at[z, y, xp, 32:64], to_xm)),
                ((b.at[z, y], to_yp), (b.at[z, y], to_ym)),
                ((b.at[z, ym, 0:2], to_yp), (b.at[z, yp, 2:4], to_ym)),
                ((b.at[z, 0:2], to_zp), (b.at[z, 2:4], to_zm)),
            )
        elif route == 1:
            refs = (
                ((b.at[z, y, x], to_yp), (b.at[z, y, x], to_ym)),
                ((b.at[z, ym, x, 0:32], to_yp), (b.at[z, yp, x, 32:64], to_ym)),
                ((b.at[z, :, x], to_xp), (b.at[z, :, x], to_xm)),
                ((b.at[z, 0:2, xm], to_xp), (b.at[z, 2:4, xp], to_xm)),
                ((b.at[z, 0:2], to_zp), (b.at[z, 2:4], to_zm)),
            )
        elif route == 2:
            refs = (
                ((b.at[z, y, x, 0:32], to_zp), (b.at[z, y, x, 32:64], to_zm)),
                ((b.at[:, y, x], to_xp), (b.at[:, y, x], to_xm)),
                ((b.at[0, y, xm], to_xp), (b.at[1, y, xp], to_xm)),
                ((b.at[:, y], to_yp), (b.at[:, y], to_ym)),
                ((b.at[0, ym], to_yp), (b.at[1, yp], to_ym)),
            )
        elif route == 3:
            refs = (
                ((b.at[z, y, x, 0:32], to_zp), (b.at[z, y, x, 32:64], to_zm)),
                ((b.at[:, y, x], to_yp), (b.at[:, y, x], to_ym)),
                ((b.at[0, ym, x], to_yp), (b.at[1, yp, x], to_ym)),
                ((b.at[:, :, x], to_xp), (b.at[:, :, x], to_xm)),
                ((b.at[0, :, xm], to_xp), (b.at[1, :, xp], to_xm)),
            )
        elif route == 4:
            refs = (
                ((b.at[z, y, x], to_xp), (b.at[z, y, x], to_xm)),
                ((b.at[z, y, xm, 0:32], to_xp), (b.at[z, y, xp, 32:64], to_xm)),
                ((b.at[z, y, 0:2], to_zp), (b.at[z, y, 2:4], to_zm)),
                ((b.at[:, y], to_yp), (b.at[:, y], to_ym)),
                ((b.at[0, ym], to_yp), (b.at[1, yp], to_ym)),
            )
        else:
            refs = (
                ((b.at[z, y, x], to_yp), (b.at[z, y, x], to_ym)),
                ((b.at[z, ym, x, 0:32], to_yp), (b.at[z, yp, x, 32:64], to_ym)),
                ((b.at[z, 0:2, x], to_zp), (b.at[z, 2:4, x], to_zm)),
                ((b.at[:, :, x], to_xp), (b.at[:, :, x], to_xm)),
                ((b.at[0, :, xm], to_xp), (b.at[1, :, xp], to_xm)),
            )
        for ref, to in refs[k]:
            send(ref, to, u, k)

    def pair(src, dst, n):
        return pltpu.make_async_remote_copy(
            src_ref=src, dst_ref=dst, send_sem=pair_sent.at[n], recv_sem=pair_arrived.at[n],
            device_id=partner, device_id_type=MESH,
        )

    def columns(n):
        return [pl.ds(512 * i, 512) for i in range(n)]

    def rows_of(h):
        at, size = GROUPS_OF_ROWS[h]
        return pl.ds(at, size)

    exchange_tokens = pair(tokens, whole.at[tp], 0)
    exchange_tokens.start()
    exchange_first = [pair(part.at[rows_of(h)], got_first.at[rows_of(h)], 1 + h) for h in (0, 1)]
    exchange_stats = [pair(stats.at[rows_of(h)], stats_got.at[rows_of(h)], 3 + h) for h in (0, 1)]
    exchange_mix = [
        [pair(part.at[rows_of(h), c], got_mix.at[rows_of(h), c], 5 + 4 * h + i)
         for i, c in enumerate(columns(4))] for h in (0, 1)
    ]
    exchange_last = [
        [pair(last_part.at[rows_of(h), c], got_last.at[rows_of(h), c], 13 + 2 * h + i)
         for i, c in enumerate(columns(2))] for h in (0, 1)
    ]

    stores = [
        pltpu.make_async_copy(last_part.at[rows_of(h)], result.at[rows_of(h)], store_sem.at[h])
        for h in (0, 1)
    ]

    def by_rows(at, size, step_rows, body):
        def one(i, carry):
            body(pl.ds(pl.multiple_of(at + i * step_rows, step_rows), step_rows))
            return carry

        lax.fori_loop(0, size // step_rows, one, 0, unroll=UNROLL if step_rows < SPAN else 1)

    def normalise(values, gain):
        factor = lax.rsqrt(jnp.mean(values * values, axis=1, keepdims=True) + EPS)
        return (values * factor * gain[...]).astype(BF)

    def norm_tokens():
        need("tokens", "first", "mix", "second", "gain", "bias", "spatial_w", "spatial_b")
        exchange_tokens.wait()

        def body(r):
            values = jnp.concatenate([whole[0, r], whole[1, r]], axis=1).astype(F32)
            normed[r] = normalise(values, norm_first)

        by_rows(0, 640, STEP_ROWS, body)

    def activate(both):
        return (silu(both[:, :128]) * both[:, 128:]).astype(BF)

    def first_hidden(u):
        for r in (pl.ds(0, 320), pl.ds(320, 320)):
            hidden[u, r] = activate(dot(normed[r], wide[u].reshape(2048, 256)))

    def down_rows(h, zi, yi):
        r = rows_of(h)
        left = jnp.concatenate([hidden[i, r] for i in range(11)], axis=1)
        right = jnp.concatenate(
            [wide[11 + j, zi, pl.ds(yi, 2)].reshape(512, 256) for j in range(5)]
            + [narrow[zi, pl.ds(yi, 2)].reshape(512, 128)], axis=1)
        return dot_t(left, right)

    def first_down(h, nb):
        part[rows_of(h), 512 * nb : 512 * nb + 512] = down_rows(h, nb // 2, 2 * (nb % 2)).astype(BF)
        if nb == 3:
            exchange_first[h].start()

    def combine_first(h):
        exchange_first[h].wait()

        def body(r):
            values = jnp.concatenate([whole[0, r], whole[1, r]], axis=1).astype(F32)
            branch = part[r].astype(F32) + got_first[r].astype(F32)
            total = (values + 0.5 * branch).astype(BF)
            middle[r] = total
            normed[r] = normalise(total.astype(F32), norm_mix)

        by_rows(*GROUPS_OF_ROWS[h], STEP_ROWS, body)

    def project_v(h):
        r = rows_of(h)
        lane = lax.broadcasted_iota(jnp.int32, (GROUPS_OF_ROWS[h][1], 128), 1)
        total = total_sq = 0.0
        for j in range(2):
            act = gelu(dot(normed[r], wide[16 + j].reshape(2048, 256)))
            v_act[r, 256 * j : 256 * j + 256] = act
            total += jnp.sum(act, axis=1, keepdims=True)
            total_sq += jnp.sum(act * act, axis=1, keepdims=True)
        stats[r] = jnp.where(lane == 0, total, jnp.where(lane == 1, total_sq, 0.0))
        exchange_stats[h].start()

    def project_u(h):
        r = rows_of(h)
        for j in range(2):
            act = gelu(dot(normed[r], wide[18 + j].reshape(2048, 256)))
            u_act[r, 256 * j : 256 * j + 256] = act

    def mix(h):
        exchange_stats[h].wait()
        row = lax.broadcasted_iota(jnp.int32, (SPAN, SPAN), 0)
        col = lax.broadcasted_iota(jnp.int32, (SPAN, SPAN), 1)

        def body(r):
            sums = stats[r] + stats_got[r]
            mean = sums[:, 0:1] * (1.0 / BW)
            var = sums[:, 1:2] * (1.0 / BW) - mean * mean
            factor = lax.rsqrt(var + EPS)
            for g in range(4):
                c = slice(128 * g, 128 * g + 128)
                v = ((v_act[r, c] - mean) * factor * ln_gain[:, c] + ln_bias[:, c]).astype(BF)
                w = jnp.where(col <= row, spatial_w[g].astype(F32), 0.0).astype(BF)
                bias = jnp.sum(
                    jnp.where(col == row, spatial_b[g : g + 1, :], 0.0), axis=1, keepdims=True)
                spatial = dot(w, v) + bias
                mixed[r, c] = (u_act[r, c] * spatial).astype(BF)

        by_rows(*GROUPS_OF_ROWS[h], SPAN, body)

    def project_out(h):
        r = rows_of(h)

        for nb in range(4):
            right = jnp.concatenate(
                [wide[20 + j, nb // 2, pl.ds(2 * (nb % 2), 2)].reshape(512, 256) for j in range(2)],
                axis=1)
            part[r, 512 * nb : 512 * nb + 512] = dot_t(mixed[r], right).astype(BF)
            if nb:
                exchange_mix[h][nb - 1].start()
        exchange_mix[h][3].start()

    def combine_mix(h):
        for block in exchange_mix[h]:
            block.wait()

        def body(r):
            branch = part[r].astype(F32) + got_mix[r].astype(F32)
            total = (middle[r].astype(F32) + branch).astype(BF)
            middle[r] = total
            normed[r] = normalise(total.astype(F32), norm_second)

        by_rows(*GROUPS_OF_ROWS[h], STEP_ROWS, body)

    def second_hidden(h):
        r = rows_of(h)

        def product(u):
            return dot(normed[r], wide[u].reshape(2048, 256))

        for u in range(11):
            hidden[u, r] = activate(product(u))

    def second_down(h):
        r = rows_of(h)
        for nb in range(2):
            c = slice(512 * nb, 512 * nb + 512)
            last_part[r, c] = down_rows(h, 1 - tp, 2 * nb).astype(BF)
            if nb:
                exchange_last[h][0].start()
        exchange_last[h][1].start()
        for nb in range(2):
            c = slice(512 * nb, 512 * nb + 512)
            part[r, c] = down_rows(h, tp, 2 * nb).astype(BF)

    def finish(h):
        for block in exchange_last[h]:
            block.wait()

        def body(r):
            own = middle[r, pl.ds(pl.multiple_of(tp * 1024, 1024), 1024)].astype(F32)
            branch = part[r, 0:1024].astype(F32) + got_last[r].astype(F32)
            last_part[r] = (own + 0.5 * branch).astype(BF)

        by_rows(*GROUPS_OF_ROWS[h], STEP_ROWS, body)
        stores[h].start()

    def task(n):
        if n == 90:
            norm_tokens()
        elif n < 120:
            first_hidden(n - 100)
        elif n < 130:
            first_down((n - 120) // 4, n % 4)
        else:
            run = (combine_first, project_v, project_u, mix, project_out)
            run[n // 10 - 13](n % 10)

    for code in PROGRAM:
        if code < 1000:
            step(code // 10, code % 10)
        else:
            task(code - 1000)
    for h in (0, 1):
        combine_mix(h)
        second_hidden(h)
        second_down(h)
    for h in (0, 1):
        finish(h)
    for u in range(N_UNITS):
        for k in range(5):
            wait_for(u, k, sent)
    for store in stores:
        store.wait()


def on_device(*args):
    (tokens, norm_first, norm_mix, norm_second, gate_w, up_w, down_w, gate_s, up_s, down_s,
     u_w, v_w, u_s, v_s, ln_gain, ln_bias, spatial_w, spatial_b, out_w, out_s) = args
    line = lambda a: a.reshape(1, -1)
    rows = tokens.shape[0]
    vmem = pltpu.VMEM
    return pl.pallas_call(
        kernel,
        out_shape=jax.ShapeDtypeStruct(tokens.shape, BF),
        in_specs=[pl.BlockSpec(memory_space=pl.ANY)] * 20,
        out_specs=pl.BlockSpec(memory_space=pl.ANY),
        scratch_shapes=[
            *[vmem((1, 2048), F32)] * 3,
            *[vmem((11, 128), F32)] * 2,
            vmem((1, 64), F32),
            *[vmem((1, 512), F32)] * 4,
            vmem((4, 128, 128), BF),
            vmem((4, 128), F32),
            vmem((1, 64), F32),
            *[vmem((64, 1408), F32)] * 3,
            *[vmem((64, 512), F32)] * 3,
            vmem((N_UNITS - 1, 2, 4, 4, 64, 256), BF),
            vmem((2, 4, 4, 64, 128), BF),
            vmem((2, rows, 1024), BF),
            vmem((rows, 2048), BF),
            vmem((rows, 2048), BF),
            vmem((11, rows, 128), BF),
            vmem((rows, 2048), BF),
            vmem((rows, 2048), BF),
            vmem((rows, 2048), BF),
            vmem((rows, 1024), BF),
            vmem((rows, 1024), BF),
            vmem((rows, 512), F32),
            vmem((rows, 512), F32),
            vmem((rows, 512), BF),
            vmem((rows, 128), F32),
            vmem((rows, 128), F32),
            pltpu.SemaphoreType.DMA((N_UNITS, 5)),
            pltpu.SemaphoreType.DMA((N_UNITS, 5)),
            *[pltpu.SemaphoreType.DMA((n,)) for n in (17, 17, 20, 2)],
        ],
        compiler_params=pltpu.CompilerParams(
            collective_id=0, has_side_effects=True, vmem_limit_bytes=67043328
        ),
    )(tokens, line(norm_first), line(norm_mix), line(norm_second), gate_w, up_w, down_w.T,
      gate_s.reshape(-1, 128), up_s.reshape(-1, 128), line(down_s), u_w, v_w, line(u_s), line(v_s), line(ln_gain),
      line(ln_bias), spatial_w, spatial_b, out_w.T, line(out_s))


def solution(mesh):
    torus = Mesh(
        mesh.devices.reshape(mesh.shape["rep"], 2, 4, 4, mesh.shape["tp"]),
        ("rep", "fs_0", "fs_1", "fs_2", "tp"),
    )
    in_specs = (
        P(REP_FS, "tp"), P(), P(), P(), P(FS, "tp"), P(FS, "tp"), P("tp", FS), P("tp"), P("tp"),
        P(FS), P(FS, "tp"), P(FS, "tp"), P("tp"), P("tp"), P("tp"), P("tp"),
        P("tp", None, None), P("tp", None), P("tp", FS), P(FS),
    )
    return jax.shard_map(
        on_device, mesh=torus, in_specs=in_specs, out_specs=P(REP_FS, "tp"), check_vma=False
    )
```
